32 devices in a mesh: sp: 8 (over z, x), dp: 4 (over y, core).
Axes of the slice: x: 2, y: 2, z: 4, core: 2. Of those that a mesh axis runs over, the one named last changes fastest.
Arguments:
- query_input: bfloat16 [4, 4096, 2048], P('dp', 'sp'), may hold values from -6 to 6
- forget_gate_input: bfloat16 [4, 4096, 2048], P('dp', 'sp'), may hold values from -6.5 to 6.5
- value_input: bfloat16 [4, 4096, 2048], P('dp', 'sp'), may hold values from -6 to 6
- gate_input: bfloat16 [4, 4096, 2048], P('dp', 'sp'), may hold values from -6 to 6
- extra_decay: bfloat16 [4, 4096, 2048], P('dp', 'sp'), may hold values from -0.7 to 0
- floor_gap: float32 [2048], replicated, may hold values from 0 to 0.06
- norm_gain: float32 [2048], replicated, may hold values from 0.1 to 1.9
- out_weight: bfloat16 [2048, 4096], P(None, 'dp'), may hold values from -0.125 to 0.125
Outputs:
- mixed_out: bfloat16 [4, 4096, 4096], P('dp', 'sp')
The draws below stay inside these ranges and needn't reach their ends.
All inputs are finite; a program needn't handle non-finite values.
Results may differ from the reference program's by a relative error of at most 0.0049.
Values may be sent and summed in bfloat16 or wider, within the bound.
A program may use at most 192 MiB of HBM per device.

```python
import jax
import jax.numpy as jnp
from jax import lax

D = 4096
HW = 2048
HEAD_DIM = 128
BLOCK = 128
TOK_DEV = 512
HEADS = 16
SEQUENCE_LENGTH = 4096
SEQS = 4


def draw_forget_gate_input(key, part):
    key_noise = jax.random.fold_in(key, 101)
    key_shift = jax.random.fold_in(key, 102)
    noise_field = jax.random.truncated_normal(key_noise, -5.0, 5.0, (SEQS, SEQUENCE_LENGTH, HW), jnp.float32)
    block_shift = jax.random.uniform(key_shift, (SEQS, SEQUENCE_LENGTH // TOK_DEV, 1, HEADS, 1), jnp.float32, -1.5, 1.5)
    block_shift = jnp.broadcast_to(block_shift, (SEQS, SEQUENCE_LENGTH // TOK_DEV, TOK_DEV, HEADS, HEAD_DIM))
    return (noise_field + block_shift.reshape(SEQS, SEQUENCE_LENGTH, HW)).astype(jnp.bfloat16)


def draw_extra_decay(key, part):
    key_stable_draw = jax.random.fold_in(key, 201)
    key_spots = jax.random.fold_in(key, 202)
    key_loss = jax.random.fold_in(key, 203)
    stable_portion = -jax.random.uniform(key_stable_draw, (SEQS, SEQUENCE_LENGTH, HW), jnp.float32) / SEQUENCE_LENGTH
    sample_places = jax.random.randint(key_spots, (SEQS, 3), 0, SEQUENCE_LENGTH)
    surge_mask = jnp.any(jnp.arange(SEQUENCE_LENGTH)[None, :, None] == sample_places[:, None, :], axis=-1)
    loss_fraction = jax.random.uniform(key_loss, (SEQS, SEQUENCE_LENGTH, HW), jnp.float32, 0.2, 0.5)
    return jnp.where(surge_mask[:, :, None], jnp.log1p(-loss_fraction), stable_portion).astype(jnp.bfloat16)


def draw_floor_gap(key, part):
    key_fast = jax.random.fold_in(key, 301)
    key_quick = jax.random.fold_in(key, 302)
    key_slow = jax.random.fold_in(key, 303)
    fast_share = 0.5
    fast_heads = jax.random.uniform(key_fast, (HEADS, 1), jnp.float32) < fast_share
    quick_gap = jnp.exp(jax.random.uniform(key_quick, (HEADS, HEAD_DIM), jnp.float32, jnp.log(0.02), jnp.log(0.06)))
    slow_gap = jnp.exp(jax.random.uniform(key_slow, (HEADS, HEAD_DIM), jnp.float32, jnp.log(0.1), 0.0)) / SEQUENCE_LENGTH
    return jnp.where(fast_heads, quick_gap, slow_gap).reshape(HW).astype(jnp.float32)


def level_of(own_key, extent, pieces, smallest, high):
    gain, own = 1.0, jax.random.fold_in(own_key, 6)
    for dim, shards_of in pieces:
        heights = jnp.exp(jax.random.uniform(jax.random.fold_in(own, dim), (shards_of,), jnp.float32, smallest / len(pieces), high / len(pieces)))
        gain = gain * jnp.repeat(heights, extent[dim] // shards_of).reshape([-1 if axis == dim else 1 for axis in range(len(extent))])
    return gain


def centred(key, dims, spread, most, shards=(), kind=jnp.bfloat16):
    values = spread * jax.random.normal(key, dims, jnp.float32)
    if shards:
        values = values * level_of(key, dims, shards, -0.22, 0.18)
    return jnp.clip(values, -most, most).astype(kind)


def setup_inputs(seed: int = 0) -> dict:
    key_of = jax.random.split(jax.random.key(seed), 9)
    query_input = centred(key_of[0], (SEQS, SEQUENCE_LENGTH, HW), 1.0, 6.0, ((0, 4), (1, 8)))
    forget_gate_input = draw_forget_gate_input(jax.random.fold_in(key_of[8], 71), 0)
    value_input = centred(key_of[2], (SEQS, SEQUENCE_LENGTH, HW), 1.0, 6.0, ((0, 4), (1, 8)))
    gate_input = centred(key_of[3], (SEQS, SEQUENCE_LENGTH, HW), 1.0, 6.0, ((0, 4), (1, 8)))
    extra_decay = draw_extra_decay(jax.random.fold_in(key_of[8], 71), 0)
    floor_gap = draw_floor_gap(jax.random.fold_in(key_of[8], 71), 0)
    norm_gain = jnp.clip(1.0 + 0.18 * jax.random.normal(key_of[6], (HW,), jnp.float32), 0.1, 1.9)
    out_weight = centred(key_of[7], (HW, D), HW ** -0.5, 0.125, ((1, 4),))
    return dict(query_input=query_input, forget_gate_input=forget_gate_input, value_input=value_input, gate_input=gate_input, extra_decay=extra_decay, floor_gap=floor_gap, norm_gain=norm_gain, out_weight=out_weight)


norm_eps = 1e-06
pairs_per_step = 16
highest = lax.Precision.HIGHEST

def prepare(query_input, forget_gate_input, value_input, extra_decay, floor_gap):
    positions, channels = query_input.shape
    head_shape = (positions, channels // HEAD_DIM, HEAD_DIM)
    queries = jax.nn.silu(query_input.astype(jnp.float32))
    inflow = floor_gap * jax.nn.sigmoid(-forget_gate_input.astype(jnp.float32))
    log_keep = jnp.log1p(-inflow) + extra_decay.astype(jnp.float32)
    value_rows = value_input.astype(jnp.float32)
    return (queries.reshape(head_shape), inflow.reshape(head_shape), log_keep.reshape(head_shape), value_rows.reshape(head_shape))

def block_parts(queries, inflow, log_keep, value_rows):
    positions, head_count, head_width = queries.shape
    block_count = positions // BLOCK
    pair_count = block_count * head_count
    causal = jnp.tril(jnp.ones((BLOCK, BLOCK), dtype=bool))

    def to_pairs(tensor):
        paired = tensor.reshape(block_count, BLOCK, head_count, head_width).transpose(0, 2, 1, 3)
        return paired.reshape(pair_count // pairs_per_step, pairs_per_step, BLOCK, head_width)

    def group_terms(operands):
        query_grp, inflow_grp, keep_grp, value_grp = operands
        running = jnp.cumsum(keep_grp, axis=1)
        decayed = query_grp * jnp.exp(running)
        boosted = inflow_grp * jnp.exp(-running)
        scores = jnp.einsum('gtk,gsk->gts', decayed, boosted, precision=highest)
        scores = jnp.where(causal[None], scores, 0.0)
        inner = jnp.einsum('gts,gsv->gtv', scores, value_grp, precision=highest)
        latest = running[:, -1, :]
        weighted = inflow_grp * jnp.exp(latest[:, None, :] - running)
        block_state = jnp.einsum('gsk,gsv->gkv', weighted, value_grp, precision=highest)
        return (inner, decayed, block_state, jnp.exp(latest))
    inner, decayed, block_state, block_fade = lax.map(group_terms, (to_pairs(queries), to_pairs(inflow), to_pairs(log_keep), to_pairs(value_rows)))
    return (inner.reshape(block_count, head_count, BLOCK, head_width), decayed.reshape(block_count, head_count, BLOCK, head_width), block_state.reshape(block_count, head_count, head_width, head_width), block_fade.reshape(block_count, head_count, head_width))

def finish(inner, decayed, prior_states, gate_input, norm_gain):
    block_count, head_count, block_len, head_width = inner.shape
    result = inner + jnp.einsum('nhtk,nhkv->nhtv', decayed, prior_states, precision=highest)
    result = result.transpose(0, 2, 1, 3).reshape(block_count * block_len, head_count, head_width)
    scaled = result * lax.rsqrt(lax.optimization_barrier(jnp.mean(result * result, axis=-1, keepdims=True)) + norm_eps)
    scaled = scaled.reshape(block_count * block_len, head_count * head_width)
    scaled = scaled * norm_gain * jax.nn.silu(gate_input.astype(jnp.float32))
    return scaled.astype(jnp.bfloat16)

def reference(query_input, forget_gate_input, value_input, gate_input, extra_decay, floor_gap, norm_gain, out_weight):

    def one_sequence(member):
        query_one, forget_one, value_one, gate_one, extra_one = member
        queries, inflow, log_keep, value_rows = prepare(query_one, forget_one, value_one, extra_one, floor_gap)
        inner, decayed, block_state, block_fade = block_parts(queries, inflow, log_keep, value_rows)

        def carry_step(state, operands):
            fresh, fading = operands
            return (fading[..., None] * state + fresh, state)
        _, prior_states = lax.scan(carry_step, jnp.zeros(block_state.shape[1:], jnp.float32), (block_state, block_fade))
        hidden = finish(inner, decayed, prior_states, gate_one, norm_gain)
        return jnp.dot(hidden, out_weight, preferred_element_type=jnp.float32).astype(jnp.bfloat16)
    return lax.map(one_sequence, (query_input, forget_gate_input, value_input, gate_input, extra_decay))
```

```python
import functools

import jax
import jax.numpy as jnp
from jax import lax
from jax.experimental import pallas as pl
from jax.experimental.pallas import tpu as pltpu
from jax.sharding import PartitionSpec as P

HEAD_DIM = 128
BLOCK = 128
GROUP = 2
norm_eps = 1e-06
bf16, f32 = jnp.bfloat16, jnp.float32


def dot(a, b, dims):
    return lax.dot_general(a, b, (dims, ((), ())), preferred_element_type=f32)


NN = ((1,), (0,))
NT = ((1,), (1,))
TN = ((0,), (0,))


def local_kernel(q_ref, f_ref, v_ref, e_ref, gap_ref, inner_ref, dec_ref, state_ref, fade_ref):
    positions, width = q_ref.shape
    rows = lax.broadcasted_iota(jnp.int32, (BLOCK, BLOCK), 0)
    cols = lax.broadcasted_iota(jnp.int32, (BLOCK, BLOCK), 1)
    causal = rows >= cols
    ones_tri = jnp.where(causal, 1.0, 0.0).astype(bf16)
    gap = gap_ref[...]
    states = [None] * (width // HEAD_DIM)
    total = jnp.zeros((1, width), f32)
    for block in range(positions // BLOCK):
        at = pl.ds(block * BLOCK, BLOCK)
        q_in = q_ref[at, :].astype(f32)
        queries = q_in / (1.0 + jnp.exp(-q_in))
        inflow = gap / (1.0 + jnp.exp(f_ref[at, :].astype(f32)))
        log_keep = jnp.log(1.0 - inflow) + e_ref[at, :].astype(f32)
        high = log_keep.astype(bf16)
        low = (log_keep - high.astype(f32)).astype(bf16)
        running = dot(ones_tri, high, NN) + dot(ones_tri, low, NN)
        latest = running[BLOCK - 1 :, :]
        decayed = queries * jnp.exp(running)
        boosted = (inflow * jnp.exp(-running)).astype(bf16)
        weighted = (inflow * jnp.exp(latest - running)).astype(bf16)
        dec_ref[at, :] = (decayed * jnp.exp(total)).astype(bf16)
        decayed = decayed.astype(bf16)
        fade = jnp.exp(latest)
        for head in range(width // HEAD_DIM):
            lanes = slice(head * HEAD_DIM, (head + 1) * HEAD_DIM)
            value = v_ref[at, lanes]
            scores = dot(decayed[:, lanes], boosted[:, lanes], NT)
            scores = jnp.where(causal, scores, 0.0).astype(bf16)
            inner = dot(scores, value, NN)
            fresh = dot(value, weighted[:, lanes], TN)
            if block:
                inner = inner + dot(decayed[:, lanes], states[head].astype(bf16), NT)
                fresh = fade[:, lanes] * states[head] + fresh
            states[head] = fresh
            inner_ref[at, lanes] = inner
        total = total + latest
    for head in range(width // HEAD_DIM):
        state_ref[head] = states[head].astype(bf16)
    fade_ref[...] = jnp.exp(total)


def finish_kernel(axis, inner_ref, dec_ref, gate_ref, gain_ref, states_ref, fades_ref, hidden_ref):
    positions, width = inner_ref.shape
    mine = lax.axis_index(axis)
    count = states_ref.shape[0]
    for head in range(width // HEAD_DIM):
        lanes = slice(head * HEAD_DIM, (head + 1) * HEAD_DIM)
        entering = jnp.zeros((HEAD_DIM, HEAD_DIM), f32)
        for other in range(count - 1):
            longer = fades_ref[other][:, lanes] * entering + states_ref[other, head].astype(f32)
            entering = jnp.where(other < mine, longer, entering)
        result = inner_ref[:, lanes] + dot(dec_ref[:, lanes], entering.astype(bf16), NT)
        mean = jnp.mean(result * result, axis=-1, keepdims=True)
        scaled = result * lax.rsqrt(mean + norm_eps) * gain_ref[:, lanes]
        gate = gate_ref[:, lanes].astype(f32)
        hidden_ref[:, lanes] = (scaled * (gate / (1.0 + jnp.exp(-gate)))).astype(bf16)


def project_kernel(hidden_ref, weight_ref, out_ref):
    pieces, _, depth, width = weight_ref.shape
    weight = weight_ref[...].reshape(pieces * depth, width)
    out_ref[...] = dot(hidden_ref[...], weight, NN).astype(out_ref.dtype)


def shards(
    query_input,
    forget_gate_input,
    value_input,
    gate_input,
    extra_decay,
    floor_gap,
    norm_gain,
    out_weight,
):
    sp, dp = lax.axis_size("sp"), lax.axis_size("dp")
    _, positions, channels = query_input.shape
    heads, width = channels // HEAD_DIM, GROUP * HEAD_DIM
    steps = heads // GROUP
    depth, columns = out_weight.shape
    piece = depth // sp

    mine = lax.dynamic_slice_in_dim(out_weight, lax.axis_index("sp") * piece, piece, axis=0)
    weights = lax.all_gather(mine, ("sp", "dp")).reshape(sp, dp, piece, columns)

    tokens = pl.BlockSpec((positions, width), lambda i: (0, i))
    params = pl.BlockSpec((1, width), lambda i: (0, i))
    state = pl.BlockSpec((GROUP, HEAD_DIM, HEAD_DIM), lambda i: (i, 0, 0))
    inner, decayed, whole_state, whole_fade = pl.pallas_call(
        local_kernel,
        grid=(steps,),
        in_specs=[tokens] * 4 + [params],
        out_specs=[tokens, tokens, state, params],
        out_shape=[
            jax.ShapeDtypeStruct((positions, channels), f32),
            jax.ShapeDtypeStruct((positions, channels), bf16),
            jax.ShapeDtypeStruct((heads, HEAD_DIM, HEAD_DIM), bf16),
            jax.ShapeDtypeStruct((1, channels), f32),
        ],
        cost_estimate=pl.CostEstimate(flops=3 * 10**9, bytes_accessed=2 * 10**7, transcendentals=10**7),
        name="local",
    )(query_input[0], forget_gate_input[0], value_input[0], extra_decay[0], floor_gap[None])

    states = lax.all_gather(whole_state, "sp")
    fades = lax.all_gather(whole_fade, "sp")

    hidden = pl.pallas_call(
        functools.partial(finish_kernel, "sp"),
        grid=(steps,),
        in_specs=[
            tokens,
            tokens,
            tokens,
            params,
            pl.BlockSpec((sp, GROUP, HEAD_DIM, HEAD_DIM), lambda i: (0, i, 0, 0)),
            pl.BlockSpec((sp, 1, width), lambda i: (0, 0, i)),
        ],
        out_specs=tokens,
        out_shape=jax.ShapeDtypeStruct((positions, channels), bf16),
        cost_estimate=pl.CostEstimate(flops=10**9, bytes_accessed=10**7, transcendentals=10**6),
        name="finish",
    )(inner, decayed, gate_input[0], norm_gain[None], states, fades)

    tile = columns // 2
    mixed = pl.pallas_call(
        project_kernel,
        grid=(dp, columns // tile),
        in_specs=[
            pl.BlockSpec((positions, channels), lambda n, c: (0, 0)),
            pl.BlockSpec((sp, 1, piece, tile), lambda n, c: (0, n, 0, c)),
        ],
        out_specs=pl.BlockSpec((positions, tile), lambda n, c: (0, n * (columns // tile) + c)),
        out_shape=jax.ShapeDtypeStruct((positions, dp * columns), bf16),
        name="project",
    )(hidden, weights)
    return mixed[None]


def solution(mesh):
    in_specs = (
        P("dp", "sp", None),
        P("dp", "sp", None),
        P("dp", "sp", None),
        P("dp", "sp", None),
        P("dp", "sp", None),
        P(),
        P(),
        P(None, "dp"),
    )
    out_specs = P("dp", "sp", None)
    return jax.shard_map(shards, mesh=mesh, in_specs=in_specs, out_specs=out_specs, check_vma=False)
```

```python
import functools

import jax
import jax.numpy as jnp
from jax import lax
from jax.experimental import pallas as pl
from jax.experimental.pallas import tpu as pltpu
from jax.sharding import PartitionSpec as P

HEAD_DIM = 128
BLOCK = 128
GROUP = 2
CORES = 2
CHUNKS = 8
FADE_ROWS = 16
norm_eps = 1e-06
bf16, f32 = jnp.bfloat16, jnp.float32


def dot(a, b, dims):
    return lax.dot_general(a, b, (dims, ((), ())), preferred_element_type=f32)


NN = ((1,), (0,))
NT = ((1,), (1,))
TN = ((0,), (0,))


def local_part(q_ref, f_ref, v_ref, e_ref, gap_ref, inner_ref, dec_ref, states_ref, step):
    positions, width = q_ref.shape
    rows = lax.broadcasted_iota(jnp.int32, (BLOCK, BLOCK), 0)
    cols = lax.broadcasted_iota(jnp.int32, (BLOCK, BLOCK), 1)
    causal = rows >= cols
    ones_tri = jnp.where(causal, 1.0, 0.0).astype(bf16)
    gap = gap_ref[...]
    states = [None] * GROUP
    total = jnp.zeros((1, width), f32)
    for block in range(positions // BLOCK):
        at = pl.ds(block * BLOCK, BLOCK)
        q_in = q_ref[at, :].astype(f32)
        queries = q_in / (1.0 + jnp.exp(-q_in))
        inflow = gap / (1.0 + jnp.exp(f_ref[at, :].astype(f32)))
        log_keep = jnp.log(1.0 - inflow) + e_ref[at, :].astype(f32)
        high = log_keep.astype(bf16)
        low = (log_keep - high.astype(f32)).astype(bf16)
        running = dot(ones_tri, high, NN) + dot(ones_tri, low, NN)
        latest = running[BLOCK - 1 :, :]
        decayed = queries * jnp.exp(running)
        boosted = (inflow * jnp.exp(-running)).astype(bf16)
        weighted = (inflow * jnp.exp(latest - running)).astype(bf16)
        dec_ref[step, at, :] = (decayed * jnp.exp(total)).astype(bf16)
        decayed = decayed.astype(bf16)
        fade = jnp.exp(latest)
        for head in range(GROUP):
            lanes = slice(head * HEAD_DIM, (head + 1) * HEAD_DIM)
            value = v_ref[at, lanes]
            scores = dot(decayed[:, lanes], boosted[:, lanes], NT)
            scores = jnp.where(causal, scores, 0.0).astype(bf16)
            inner = dot(scores, value, NN)
            fresh = dot(value, weighted[:, lanes], TN)
            if block:
                inner = inner + dot(decayed[:, lanes], states[head].astype(bf16), NT)
                fresh = fade[:, lanes] * states[head] + fresh
            states[head] = fresh
            inner_ref[step, at, lanes] = inner
        total = total + latest
    fade = jnp.exp(total)
    high = fade.astype(bf16).astype(f32)
    first = lax.broadcasted_iota(jnp.int32, (FADE_ROWS, width), 0) == 0
    fade = jnp.where(first, high, fade - high).astype(bf16)
    for head in range(GROUP):
        lanes = slice(head * HEAD_DIM, (head + 1) * HEAD_DIM)
        states_ref[step * GROUP + head, :HEAD_DIM, :] = states[head].astype(bf16)
        states_ref[step * GROUP + head, HEAD_DIM:, :] = fade[:, lanes]


def finish_part(gate_ref, gain_ref, inner_ref, dec_ref, enter_ref, hidden_ref, step):
    sp, own_heads = enter_ref.shape[:2]
    mine = lax.axis_index("sp")
    for head in range(GROUP):
        lanes = slice(head * HEAD_DIM, (head + 1) * HEAD_DIM)
        number = step * GROUP + head
        slot = lax.rem(mine - number // own_heads + sp, sp)
        entering = enter_ref[slot, lax.rem(number, own_heads)]
        result = inner_ref[step, :, lanes] + dot(dec_ref[step, :, lanes], entering, NT)
        mean = jnp.mean(result * result, axis=-1, keepdims=True)
        scaled = result * lax.rsqrt(mean + norm_eps) * gain_ref[:, lanes]
        gate = gate_ref[:, lanes].astype(f32)
        hidden_ref[:, lanes] = (scaled * (gate / (1.0 + jnp.exp(-gate)))).astype(bf16)


def remote(src, dst, send, recv, device):
    return pltpu.make_async_remote_copy(
        src_ref=src,
        dst_ref=dst,
        send_sem=send,
        recv_sem=recv,
        device_id=device,
        device_id_type=pl.DeviceIdType.MESH,
    )


def fused_kernel(
    sp,
    dp,
    q_ref,
    f_ref,
    v_ref,
    e_ref,
    gate_ref,
    gap_ref,
    gain_ref,
    w_ref,
    hidden_ref,
    all_ref,
    inner_ref,
    dec_ref,
    states_ref,
    given_ref,
    prior_ref,
    enter_ref,
    local_sem,
    own_sems,
    y_send,
    y_recv,
    x_send,
    x_recv,
    s1_send,
    s1_recv,
    s2_send,
    s2_recv,
    a_send,
    a_recv,
    b_send,
    b_recv,
):
    now = pl.program_id(0)
    last = pl.num_programs(0) - 1
    steps = inner_ref.shape[0]
    own_heads = given_ref.shape[1]
    i, j = lax.axis_index("sp"), lax.axis_index("dp")
    far = dp // CORES
    y, core = j // CORES, lax.rem(j, CORES)
    half = lax.rem(i, 2)
    partner = i + 1 - 2 * half
    sibling = y * CORES + 1 - core
    depth = w_ref.shape[0]
    chunk = depth // 2 // CHUNKS

    def rows(side, k):
        return pl.ds(pl.multiple_of(side * (depth // 2) + k * chunk, chunk), chunk)

    def block_of(offset, of_core):
        return lax.rem(y - offset + far, far) * CORES + of_core

    def over_y(offset, k):
        to = lax.rem(y + offset, far) * CORES + core
        at = rows(half, k)
        sems = (y_send.at[offset - 1, k], y_recv.at[offset - 1, k])
        return remote(w_ref.at[at], all_ref.at[j, at], *sems, {"sp": i, "dp": to})

    def forward(offset, k, side, of_core, send, recv, device):
        piece = all_ref.at[block_of(offset, of_core), rows(side, k)]
        return remote(piece, piece, send.at[offset - 1, k], recv.at[offset - 1, k], device)

    over_x = lambda o, k, side: forward(o, k, side, core, x_send, x_recv, {"sp": partner, "dp": j})
    beside = {"sp": i, "dp": sibling}
    near = lambda o, k, of_core: forward(o, k, half, of_core, s1_send, s1_recv, beside)
    other = lambda o, k, of_core: forward(o, k, 1 - half, of_core, s2_send, s2_recv, beside)
    own_near = remote(w_ref, all_ref.at[j], own_sems.at[0], own_sems.at[1], beside)
    from_near = remote(w_ref, all_ref.at[sibling], own_sems.at[0], own_sems.at[1], beside)
    keep = pltpu.make_async_copy(w_ref, all_ref.at[j], local_sem)
    pieces = [(o, k) for k in range(CHUNKS) for o in range(1, far)]

    def give(d):
        to = lax.rem(i + d, sp)
        part = states_ref.at[pl.ds(to * own_heads, own_heads)]
        return remote(part, given_ref.at[d], a_send.at[d], a_recv.at[d], {"sp": to, "dp": j})

    def back(d):
        to = lax.rem(i + d, sp)
        return remote(prior_ref.at[d], enter_ref.at[d], b_send.at[d], b_recv.at[d], {"sp": to, "dp": j})

    @pl.when(now == 0)
    def _():
        barrier = pltpu.get_barrier_semaphore()
        for o in range(1, far):
            to = lax.rem(y + o, far) * CORES + core
            pl.semaphore_signal(barrier, 1, device_id={"sp": i, "dp": to}, device_id_type=pl.DeviceIdType.MESH)
        pl.semaphore_signal(barrier, 1, device_id=beside, device_id_type=pl.DeviceIdType.MESH)
        for d in range(1, sp):
            to = lax.rem(i + d, sp)
            pl.semaphore_signal(barrier, 1, device_id={"sp": to, "dp": j}, device_id_type=pl.DeviceIdType.MESH)
        pl.semaphore_wait(barrier, far - 1 + 1 + sp - 1)
        for o, k in pieces:
            over_y(o, k).start()
        own_near.start()
        keep.start()

    @pl.when(now < steps)
    def _():
        local_part(q_ref, f_ref, v_ref, e_ref, gap_ref, inner_ref, dec_ref, states_ref, now)

    @pl.when(now == steps)
    def _():
        for d in range(1, sp):
            give(d).start()
        given_ref[0] = states_ref[pl.ds(i * own_heads, own_heads)]
        for d in range(1, sp):
            give(d).wait_recv()
        for head in range(own_heads):
            entering = jnp.zeros((HEAD_DIM, HEAD_DIM), f32)
            for source in range(sp):
                prior_ref[lax.rem(source - i + sp, sp), head] = entering.astype(bf16)
                slot = lax.rem(i - source + sp, sp)
                fade = given_ref[slot, head, HEAD_DIM:, :].astype(f32)
                fade = fade[0:1] + fade[1:2]
                entering = fade * entering + given_ref[slot, head, :HEAD_DIM, :].astype(f32)
        for d in range(1, sp):
            back(d).start()
        enter_ref[0] = prior_ref[0]
        for d in range(1, sp):
            back(d).wait_recv()

    @pl.when(now >= steps)
    def _():
        finish_part(gate_ref, gain_ref, inner_ref, dec_ref, enter_ref, hidden_ref, now - steps)

    for k in range(CHUNKS):
        @pl.when(now == min(2 * steps - 1, 2 * steps * k // CHUNKS + 3))
        def _():
            for o in range(1, far):
                over_y_in = forward(o, k, half, core, y_send, y_recv, beside)
                over_y_in.wait_recv()
                over_x(o, k, half).start()
                near(o, k, core).start()

    @pl.when(now == last)
    def _():
        for o, k in pieces:
            over_x(o, k, 1 - half).wait_recv()
            other(o, k, core).start()
        keep.wait()
        own_near.wait_send()
        from_near.wait_recv()
        for o, k in pieces:
            over_y(o, k).wait_send()
            over_x(o, k, half).wait_send()
            near(o, k, core).wait_send()
            near(o, k, 1 - core).wait_recv()
        for d in range(1, sp):
            give(d).wait_send()
            back(d).wait_send()
        for o, k in pieces:
            other(o, k, core).wait_send()
            other(o, k, 1 - core).wait_recv()


def project_kernel(hidden_ref, weight_ref, out_ref):
    out_ref[...] = dot(hidden_ref[...], weight_ref[0], NN).astype(out_ref.dtype)


def shards(
    query_input,
    forget_gate_input,
    value_input,
    gate_input,
    extra_decay,
    floor_gap,
    norm_gain,
    out_weight,
):
    sp, dp = lax.axis_size("sp"), lax.axis_size("dp")
    _, positions, channels = query_input.shape
    heads, width = channels // HEAD_DIM, GROUP * HEAD_DIM
    steps, own_heads = heads // GROUP, heads // sp
    depth, columns = out_weight.shape
    far = dp // CORES

    early = lambda s: (0, jnp.minimum(s, steps - 1))
    late = lambda s: (0, jnp.maximum(s - steps, 0))
    tokens = pl.BlockSpec((positions, width), early)
    after = pl.BlockSpec((positions, width), late)
    dma = pltpu.SemaphoreType.DMA
    flow = [dma((max(far - 1, 1), CHUNKS))] * 8
    packed = HEAD_DIM + FADE_ROWS
    hidden, weights = pl.pallas_call(
        functools.partial(fused_kernel, sp, dp),
        grid=(2 * steps,),
        in_specs=[tokens] * 4
        + [
            after,
            pl.BlockSpec((1, width), early),
            pl.BlockSpec((1, width), late),
            pl.BlockSpec((depth, columns), lambda s: (0, 0)),
        ],
        out_specs=[after, pl.BlockSpec(memory_space=pl.ANY)],
        out_shape=[
            jax.ShapeDtypeStruct((positions, channels), bf16),
            jax.ShapeDtypeStruct((dp, depth, columns), bf16),
        ],
        scratch_shapes=[
            pltpu.VMEM((steps, positions, width), f32),
            pltpu.VMEM((steps, positions, width), bf16),
            pltpu.VMEM((heads, packed, HEAD_DIM), bf16),
            pltpu.VMEM((sp, own_heads, packed, HEAD_DIM), bf16),
            pltpu.VMEM((sp, own_heads, HEAD_DIM, HEAD_DIM), bf16),
            pltpu.VMEM((sp, own_heads, HEAD_DIM, HEAD_DIM), bf16),
            dma,
            dma((2,)),
            *flow,
            *[dma((sp,))] * 4,
        ],
        compiler_params=pltpu.CompilerParams(
            collective_id=0,
            has_side_effects=True,
            dimension_semantics=("arbitrary",),
            vmem_limit_bytes=48 * 2**20,
        ),
        name="fused",
    )(
        query_input[0],
        forget_gate_input[0],
        value_input[0],
        extra_decay[0],
        gate_input[0],
        floor_gap[None],
        norm_gain[None],
        out_weight,
    )

    parts = 2
    tile = columns // parts
    mixed = pl.pallas_call(
        project_kernel,
        grid=(dp, parts),
        in_specs=[
            pl.BlockSpec((positions, channels), lambda n, c: (0, 0)),
            pl.BlockSpec((1, depth, tile), lambda n, c: (n, 0, c)),
        ],
        out_specs=pl.BlockSpec((positions, tile), lambda n, c: (0, n * parts + c)),
        out_shape=jax.ShapeDtypeStruct((positions, dp * columns), bf16),
        name="project",
    )(hidden, weights)
    return mixed[None]


def solution(mesh):
    in_specs = (
        P("dp", "sp", None),
        P("dp", "sp", None),
        P("dp", "sp", None),
        P("dp", "sp", None),
        P("dp", "sp", None),
        P(),
        P(),
        P(None, "dp"),
    )
    out_specs = P("dp", "sp", None)
    return jax.shard_map(shards, mesh=mesh, in_specs=in_specs, out_specs=out_specs, check_vma=False)
```

```python
import functools

import jax
import jax.numpy as jnp
from jax import lax
from jax.experimental import pallas as pl
from jax.experimental.pallas import tpu as pltpu
from jax.sharding import PartitionSpec as P

HEAD_DIM = 128
BLOCK = 128
GROUP = 2
CORES = 2
CHUNKS = 8
FADE_ROWS = 16
norm_eps = 1e-06
bf16, f32 = jnp.bfloat16, jnp.float32


def dot(a, b, dims):
    return lax.dot_general(a, b, (dims, ((), ())), preferred_element_type=f32)


NN = ((1,), (0,))
NT = ((1,), (1,))
TN = ((0,), (0,))


def local_part(q_ref, f_ref, v_ref, e_ref, gap_ref, inner_ref, dec_ref, states_ref, step):
    positions, width = q_ref.shape
    rows = lax.broadcasted_iota(jnp.int32, (BLOCK, BLOCK), 0)
    cols = lax.broadcasted_iota(jnp.int32, (BLOCK, BLOCK), 1)
    causal = rows >= cols
    ones_tri = jnp.where(causal, 1.0, 0.0).astype(bf16)
    gap = gap_ref[...]
    states = [None] * GROUP
    total = jnp.zeros((1, width), f32)
    for block in range(positions // BLOCK):
        at = pl.ds(block * BLOCK, BLOCK)
        q_in = q_ref[at, :].astype(f32)
        queries = q_in / (1.0 + jnp.exp(-q_in))
        inflow = gap / (1.0 + jnp.exp(f_ref[at, :].astype(f32)))
        log_keep = jnp.log(1.0 - inflow) + e_ref[at, :].astype(f32)
        high = log_keep.astype(bf16)
        low = (log_keep - high.astype(f32)).astype(bf16)
        running = dot(ones_tri, high, NN) + dot(ones_tri, low, NN)
        latest = running[BLOCK - 1 :, :]
        decayed = queries * jnp.exp(running)
        boosted = (inflow * jnp.exp(-running)).astype(bf16)
        weighted = (inflow * jnp.exp(latest - running)).astype(bf16)
        dec_ref[step, at, :] = (decayed * jnp.exp(total)).astype(bf16)
        decayed = decayed.astype(bf16)
        fade = jnp.exp(latest)
        for head in range(GROUP):
            lanes = slice(head * HEAD_DIM, (head + 1) * HEAD_DIM)
            value = v_ref[at, lanes]
            scores = dot(decayed[:, lanes], boosted[:, lanes], NT)
            scores = jnp.where(causal, scores, 0.0).astype(bf16)
            inner = dot(scores, value, NN)
            fresh = dot(value, weighted[:, lanes], TN)
            if block:
                inner = inner + dot(decayed[:, lanes], states[head].astype(bf16), NT)
                fresh = fade[:, lanes] * states[head] + fresh
            states[head] = fresh
            inner_ref[step, at, lanes] = inner
        total = total + latest
    fade = jnp.exp(total)
    high = fade.astype(bf16).astype(f32)
    first = lax.broadcasted_iota(jnp.int32, (FADE_ROWS, width), 0) == 0
    fade = jnp.where(first, high, fade - high).astype(bf16)
    for head in range(GROUP):
        lanes = slice(head * HEAD_DIM, (head + 1) * HEAD_DIM)
        states_ref[step * GROUP + head, :HEAD_DIM, :] = states[head].astype(bf16)
        states_ref[step * GROUP + head, HEAD_DIM:, :] = fade[:, lanes]


def finish_part(gate_ref, gain_ref, inner_ref, dec_ref, enter_ref, hidden_ref, step):
    sp, own_heads = enter_ref.shape[:2]
    mine = lax.axis_index("sp")
    for head in range(GROUP):
        lanes = slice(head * HEAD_DIM, (head + 1) * HEAD_DIM)
        number = step * GROUP + head
        slot = lax.rem(mine - number // own_heads + sp, sp)
        entering = enter_ref[slot, lax.rem(number, own_heads)]
        result = inner_ref[step, :, lanes] + dot(dec_ref[step, :, lanes], entering, NT)
        mean = jnp.mean(result * result, axis=-1, keepdims=True)
        scaled = result * lax.rsqrt(mean + norm_eps) * gain_ref[:, lanes]
        gate = gate_ref[:, lanes].astype(f32)
        hidden_ref[:, lanes] = (scaled * (gate / (1.0 + jnp.exp(-gate)))).astype(bf16)


def remote(src, dst, send, recv, device):
    return pltpu.make_async_remote_copy(
        src_ref=src,
        dst_ref=dst,
        send_sem=send,
        recv_sem=recv,
        device_id=device,
        device_id_type=pl.DeviceIdType.MESH,
    )


def fused_kernel(
    sp,
    dp,
    q_ref,
    f_ref,
    v_ref,
    e_ref,
    gate_ref,
    gap_ref,
    gain_ref,
    w_ref,
    hidden_ref,
    all_ref,
    inner_ref,
    dec_ref,
    states_ref,
    given_ref,
    prior_ref,
    enter_ref,
    local_sem,
    own_sems,
    y_send,
    y_recv,
    x_send,
    x_recv,
    s1_send,
    s1_recv,
    s2_send,
    s2_recv,
    a_send,
    a_recv,
    b_send,
    b_recv,
):
    now = pl.program_id(0)
    last = pl.num_programs(0) - 1
    steps = inner_ref.shape[0]
    own_heads = given_ref.shape[1]
    i, j = lax.axis_index("sp"), lax.axis_index("dp")
    far = dp // CORES
    y, core = j // CORES, lax.rem(j, CORES)
    half = lax.rem(i, 2)
    partner = i + 1 - 2 * half
    sibling = y * CORES + 1 - core
    depth = w_ref.shape[0]
    chunk = depth // 2 // CHUNKS

    def rows(side, k):
        return pl.ds(pl.multiple_of(side * (depth // 2) + k * chunk, chunk), chunk)

    def block_of(offset, of_core):
        return lax.rem(y - offset + far, far) * CORES + of_core

    def over_y(offset, k):
        to = lax.rem(y + offset, far) * CORES + core
        at = rows(half, k)
        sems = (y_send.at[offset - 1, k], y_recv.at[offset - 1, k])
        return remote(w_ref.at[at], all_ref.at[j, at], *sems, {"sp": i, "dp": to})

    def forward(offset, k, side, of_core, send, recv, device):
        piece = all_ref.at[block_of(offset, of_core), rows(side, k)]
        return remote(piece, piece, send.at[offset - 1, k], recv.at[offset - 1, k], device)

    over_x = lambda o, k, side: forward(o, k, side, core, x_send, x_recv, {"sp": partner, "dp": j})
    beside = {"sp": i, "dp": sibling}
    near = lambda o, k, of_core: forward(o, k, half, of_core, s1_send, s1_recv, beside)
    other = lambda o, k, of_core: forward(o, k, 1 - half, of_core, s2_send, s2_recv, beside)
    own_near = remote(w_ref, all_ref.at[j], own_sems.at[0], own_sems.at[1], beside)
    from_near = remote(w_ref, all_ref.at[sibling], own_sems.at[0], own_sems.at[1], beside)
    keep = pltpu.make_async_copy(w_ref, all_ref.at[j], local_sem)
    pieces = [(o, k) for k in range(CHUNKS) for o in range(1, far)]

    def give(d):
        to = lax.rem(i + d, sp)
        part = states_ref.at[pl.ds(to * own_heads, own_heads)]
        return remote(part, given_ref.at[d], a_send.at[d], a_recv.at[d], {"sp": to, "dp": j})

    def back(d):
        to = lax.rem(i + d, sp)
        return remote(prior_ref.at[d], enter_ref.at[d], b_send.at[d], b_recv.at[d], {"sp": to, "dp": j})

    @pl.when(now == 0)
    def _():
        barrier = pltpu.get_barrier_semaphore()
        for o in range(1, far):
            to = lax.rem(y + o, far) * CORES + core
            pl.semaphore_signal(barrier, 1, device_id={"sp": i, "dp": to}, device_id_type=pl.DeviceIdType.MESH)
        pl.semaphore_signal(barrier, 1, device_id=beside, device_id_type=pl.DeviceIdType.MESH)
        for d in range(1, sp):
            to = lax.rem(i + d, sp)
            pl.semaphore_signal(barrier, 1, device_id={"sp": to, "dp": j}, device_id_type=pl.DeviceIdType.MESH)
        pl.semaphore_wait(barrier, far - 1 + 1 + sp - 1)
        for o, k in pieces:
            over_y(o, k).start()
        own_near.start()
        keep.start()

    @pl.when(now < steps)
    def _():
        local_part(q_ref, f_ref, v_ref, e_ref, gap_ref, inner_ref, dec_ref, states_ref, now)

    @pl.when(now == steps)
    def _():
        for d in range(1, sp):
            give(d).start()
        given_ref[0] = states_ref[pl.ds(i * own_heads, own_heads)]
        for d in range(1, sp):
            give(d).wait_recv()
        for head in range(own_heads):
            entering = jnp.zeros((HEAD_DIM, HEAD_DIM), f32)
            for source in range(sp):
                prior_ref[lax.rem(source - i + sp, sp), head] = entering.astype(bf16)
                slot = lax.rem(i - source + sp, sp)
                fade = given_ref[slot, head, HEAD_DIM:, :].astype(f32)
                fade = fade[0:1] + fade[1:2]
                entering = fade * entering + given_ref[slot, head, :HEAD_DIM, :].astype(f32)
        for d in range(1, sp):
            back(d).start()
        enter_ref[0] = prior_ref[0]
        for d in range(1, sp):
            back(d).wait_recv()

    @pl.when(now >= steps)
    def _():
        finish_part(gate_ref, gain_ref, inner_ref, dec_ref, enter_ref, hidden_ref, now - steps)

    for k in range(CHUNKS):
        @pl.when(now == min(2 * steps - 1, 2 * steps * k // CHUNKS + 3))
        def _():
            for o in range(1, far):
                over_y_in = forward(o, k, half, core, y_send, y_recv, beside)
                over_y_in.wait_recv()
                over_x(o, k, half).start()
                near(o, k, core).start()

    @pl.when(now == last)
    def _():
        for o, k in pieces:
            over_x(o, k, 1 - half).wait_recv()
            other(o, k, core).start()
        keep.wait()
        own_near.wait_send()
        from_near.wait_recv()
        for o, k in pieces:
            over_y(o, k).wait_send()
            over_x(o, k, half).wait_send()
            near(o, k, core).wait_send()
            near(o, k, 1 - core).wait_recv()
        for d in range(1, sp):
            give(d).wait_send()
            back(d).wait_send()
        for o, k in pieces:
            other(o, k, core).wait_send()
            other(o, k, 1 - core).wait_recv()


def project_kernel(hidden_ref, weight_ref, out_ref):
    out_ref[...] = dot(hidden_ref[...], weight_ref[0], NN).astype(out_ref.dtype)


def shards(
    query_input,
    forget_gate_input,
    value_input,
    gate_input,
    extra_decay,
    floor_gap,
    norm_gain,
    out_weight,
):
    sp, dp = lax.axis_size("sp"), lax.axis_size("dp")
    _, positions, channels = query_input.shape
    heads, width = channels // HEAD_DIM, GROUP * HEAD_DIM
    steps, own_heads = heads // GROUP, heads // sp
    depth, columns = out_weight.shape
    far = dp // CORES

    early = lambda s: (0, jnp.minimum(s, steps - 1))
    late = lambda s: (0, jnp.maximum(s - steps, 0))
    tokens = pl.BlockSpec((positions, width), early)
    after = pl.BlockSpec((positions, width), late)
    dma = pltpu.SemaphoreType.DMA
    flow = [dma((max(far - 1, 1), CHUNKS))] * 8
    packed = HEAD_DIM + FADE_ROWS
    hidden, weights = pl.pallas_call(
        functools.partial(fused_kernel, sp, dp),
        grid=(2 * steps,),
        in_specs=[tokens] * 4
        + [
            after,
            pl.BlockSpec((1, width), early),
            pl.BlockSpec((1, width), late),
            pl.BlockSpec((depth, columns), lambda s: (0, 0)),
        ],
        out_specs=[after, pl.BlockSpec(memory_space=pl.ANY)],
        out_shape=[
            jax.ShapeDtypeStruct((positions, channels), bf16),
            jax.ShapeDtypeStruct((dp, depth, columns), bf16),
        ],
        scratch_shapes=[
            pltpu.VMEM((steps, positions, width), f32),
            pltpu.VMEM((steps, positions, width), bf16),
            pltpu.VMEM((heads, packed, HEAD_DIM), bf16),
            pltpu.VMEM((sp, own_heads, packed, HEAD_DIM), bf16),
            pltpu.VMEM((sp, own_heads, HEAD_DIM, HEAD_DIM), bf16),
            pltpu.VMEM((sp, own_heads, HEAD_DIM, HEAD_DIM), bf16),
            dma,
            dma((2,)),
            *flow,
            *[dma((sp,))] * 4,
        ],
        compiler_params=pltpu.CompilerParams(
            collective_id=0,
            has_side_effects=True,
            dimension_semantics=("arbitrary",),
            vmem_limit_bytes=63 * 2**20,
        ),
        name="fused",
    )(
        query_input[0],
        forget_gate_input[0],
        value_input[0],
        extra_decay[0],
        gate_input[0],
        floor_gap[None],
        norm_gain[None],
        out_weight,
    )

    parts = 2
    tile = columns // parts
    mixed = pl.pallas_call(
        project_kernel,
        grid=(dp, parts),
        in_specs=[
            pl.BlockSpec((positions, channels), lambda n, c: (0, 0)),
            pl.BlockSpec((1, depth, tile), lambda n, c: (n, 0, c)),
        ],
        out_specs=pl.BlockSpec((positions, tile), lambda n, c: (0, n * parts + c)),
        out_shape=jax.ShapeDtypeStruct((positions, dp * columns), bf16),
        compiler_params=pltpu.CompilerParams(vmem_limit_bytes=63 * 2**20),
        name="project",
    )(hidden, weights)
    return mixed[None]


def solution(mesh):
    in_specs = (
        P("dp", "sp", None),
        P("dp", "sp", None),
        P("dp", "sp", None),
        P("dp", "sp", None),
        P("dp", "sp", None),
        P(),
        P(),
        P(None, "dp"),
    )
    out_specs = P("dp", "sp", None)
    return jax.shard_map(shards, mesh=mesh, in_specs=in_specs, out_specs=out_specs, check_vma=False)
```
